32 devices in a mesh: ep: 4 (over z), tp: 8 (over y, x, core).
Axes of the slice: x: 2, y: 2, z: 4, core: 2. Of those that a mesh axis runs over, the one named last changes fastest.
Arguments:
- tokens: bfloat16 [512, 2048], P('ep', 'tp'), may hold values from -6 to 6
- routes: int32 [512, 2], P('ep'), may hold values from 0 to 3, as said below
- route_weights: float32 [512, 2], P('ep'), may hold values from 0.1 to 1
- grad_out: bfloat16 [512, 2048], P('ep', 'tp'), may hold values from -6 to 6
- w_gate: bfloat16 [4, 2048, 2048], P('ep', 'tp'), may hold values from -0.125 to 0.125
- w_up: bfloat16 [4, 2048, 2048], P('ep', 'tp'), may hold values from -0.125 to 0.125
- w_down: bfloat16 [4, 2048, 2048], P('ep', 'tp')
Outputs:
- grad_tokens: bfloat16 [512, 2048], P('ep', 'tp')
- grad_route: float32 [512, 2], P('ep')
- grad_gate: float32 [4, 2048, 2048], P('ep', 'tp')
- grad_up: float32 [4, 2048, 2048], P('ep', 'tp')
- grad_down: float32 [4, 2048, 2048], P('ep', 'tp')
- gate_row_norms: float32 [4, 2048], P('ep')
- up_row_norms: float32 [4, 2048], P('ep')
- down_row_norms: float32 [4, 2048], P('ep', 'tp')
The draws below stay inside these ranges and needn't reach their ends.
Inputs may be any that keep to these rules, and one draw needn't show every extreme that they name: `routes`: each token names two different experts of one group: group g holds experts g * 4 to g * 4 + 3. Among the 128 rows of one device along ep no expert is named more than 64 times, and in every draw some expert is named exactly 64 times by the rows of every device along ep.
All inputs are finite; a program needn't handle non-finite values.
Results may differ from the reference program's by a relative error of at most 0.017.
Values may be sent and summed in bfloat16 or wider, within the bound.
A program may use at most 64 MiB of HBM per device.

```python
import jax
import jax.numpy as jnp
from jax import lax

D = 2048
FF = 2048
TOP = 2
GROUP_SIZE = 4
TOK_DEV = 128
EXPERTS = 4
TOKENS = 512
CAP = 64
N_EP = 4
N_TP = 8


def permute_four(sub_key):
    return jax.random.permutation(sub_key, GROUP_SIZE)


def draw_routes(key, part):
    group_total = EXPERTS // GROUP_SIZE
    hot_group = jax.random.randint(jax.random.fold_in(key, 11), (), 0, group_total)
    hot_count = 2 * CAP
    remaining = TOK_DEV - hot_count
    if group_total > 1:
        even_share = remaining // (group_total - 1)
        leftover = remaining % (group_total - 1)
        other_counts = even_share + (jnp.arange(group_total - 1) < leftover).astype(jnp.int32)
        by_rank = jnp.concatenate([jnp.array([hot_count], jnp.int32), other_counts.astype(jnp.int32)])
    else:
        by_rank = jnp.array([hot_count], jnp.int32)
    pair_table = jnp.array([[0, 1], [2, 3], [0, 2], [1, 3], [0, 3], [1, 2]], jnp.int32)

    def one_block(block_key):
        sub_keys = jax.random.split(block_key, 4)
        group_order = jax.random.permutation(sub_keys[0], group_total)
        first_group = group_order[0]
        group_order = jnp.where(group_order == hot_group, first_group, group_order)
        group_order = group_order.at[0].set(hot_group)
        group_counts = jnp.zeros((group_total,), jnp.int32).at[group_order].set(by_rank)
        group_ends = jnp.cumsum(group_counts)
        group_starts = group_ends - group_counts
        positions = jnp.arange(TOK_DEV, dtype=jnp.int32)
        group_of = jnp.sum((positions[:, None] >= group_ends[None, :]).astype(jnp.int32), axis=1)
        within = positions - group_starts[group_of]
        pair_rows = pair_table[within % 6]
        inner_perm = jax.vmap(permute_four)(jax.random.split(sub_keys[1], group_total))
        chosen = jnp.take_along_axis(inner_perm[group_of], pair_rows, axis=1)
        swap_bit = jax.random.randint(sub_keys[2], (TOK_DEV, 1), 0, 2)
        chosen = jnp.where(swap_bit == 1, chosen[:, ::-1], chosen)
        expert_ids = group_of[:, None] * GROUP_SIZE + chosen
        shuffle = jax.random.permutation(sub_keys[3], TOK_DEV)
        return expert_ids[shuffle]
    all_blocks = jax.vmap(one_block)(jax.random.split(jax.random.fold_in(key, 12), N_EP))
    return all_blocks.reshape(TOKENS, 2).astype(jnp.int32)


def draw_w_down(key, part):
    noise = jnp.clip(jax.random.normal(jax.random.fold_in(key, 21), (EXPERTS, FF, D), jnp.float32), -6.0, 6.0)
    ramp = 3.0 ** (jnp.arange(FF, dtype=jnp.float32) / FF)
    jitter = jnp.exp(jax.random.uniform(jax.random.fold_in(key, 23), (EXPERTS, FF, 1), jnp.float32, -0.7, 0.7))
    row_scale = ramp[None, :, None] * jitter / jnp.sqrt(jnp.mean(ramp * ramp))
    return (noise * row_scale * FF ** (-0.5)).astype(jnp.bfloat16)


def block_levels(rng, extent, cuts, low, top_value):
    def one(axis_at, shards_of):
        draws = jax.random.uniform(jax.random.fold_in(jax.random.fold_in(rng, 6), axis_at), (shards_of,), jnp.float32, low / len(cuts), top_value / len(cuts))
        return jnp.repeat(jnp.exp(draws), extent[axis_at] // shards_of).reshape((-1,) + (1,) * (len(extent) - axis_at - 1))

    level = one(*cuts[0])
    for cut in cuts[1:]:
        level = level * one(*cut)
    return level


def normal_values(own_key, shape, scale, reach, cuts=(), held_as=jnp.bfloat16):
    result = jax.random.normal(own_key, shape, jnp.float32) * scale
    if len(cuts) > 0:
        result = block_levels(own_key, shape, cuts, -0.22, 0.18) * result
    return jnp.clip(result, min=-reach, max=reach).astype(held_as)


def setup_inputs(seed: int = 0) -> dict:
    key_list = jax.random.split(jax.random.key(seed), 8)
    tokens = normal_values(key_list[0], (TOKENS, D), 1.0, 6.0, ((0, 4), (1, 8)))
    routes = draw_routes(jax.random.fold_in(key_list[7], 71), 0)
    route_weights = jnp.clip(0.1 + 0.9 * jax.random.uniform(key_list[2], (TOKENS, TOP), jnp.float32) ** block_levels(key_list[2], (TOKENS, TOP), ((0, 4),), -0.2, 0.2), 0.1, 1.0)
    grad_out = normal_values(key_list[3], (TOKENS, D), 1.0, 6.0, ((0, 4), (1, 8)))
    w_gate = normal_values(key_list[4], (EXPERTS, FF, D), D ** -0.5, 0.125, ((0, 4), (1, 8)))
    w_up = normal_values(key_list[5], (EXPERTS, FF, D), D ** -0.5, 0.125, ((0, 4), (1, 8)))
    w_down = draw_w_down(jax.random.fold_in(key_list[7], 71), 0)
    return {"tokens": tokens, "routes": routes, "route_weights": route_weights, "grad_out": grad_out, "w_gate": w_gate, "w_up": w_up, "w_down": w_down}


def silu_parts(pre_act):
    sigmoid_val = jax.nn.sigmoid(pre_act)
    return pre_act * sigmoid_val, sigmoid_val * (1.0 + pre_act * (1.0 - sigmoid_val))


def reference(tokens, routes, route_weights, grad_out, w_gate, w_up, w_down):
    token_total, model_width = tokens.shape
    hidden_width = w_gate.shape[1]
    flat_ids = routes.reshape(-1).astype(jnp.int32)
    slot_total = flat_ids.shape[0]
    one_hot = (flat_ids[:, None] == jnp.arange(EXPERTS, dtype=jnp.int32)[None, :]).astype(jnp.int32)
    blocked = one_hot.reshape(N_EP, slot_total // N_EP, EXPERTS)
    earlier = jnp.cumsum(blocked, axis=1) - blocked
    slot_ids = jnp.sum(earlier * blocked, axis=2).reshape(-1).astype(jnp.int32)
    source = (jnp.arange(slot_total, dtype=jnp.int32) // (slot_total // N_EP)).astype(jnp.int32)
    position = (source * CAP + slot_ids).astype(jnp.int32)
    index_table = jnp.full((EXPERTS, N_EP * CAP), slot_total, jnp.int32)
    index_table = index_table.at[flat_ids, position].set(jnp.arange(slot_total, dtype=jnp.int32))
    weight_flat = route_weights.reshape(-1)
    zero_row = jnp.zeros((1, model_width), jnp.bfloat16)
    token_rows = jnp.concatenate([jnp.repeat(tokens, 2, axis=0), zero_row], axis=0)
    scaled = (weight_flat[:, None] * jnp.repeat(grad_out, 2, axis=0).astype(jnp.float32)).astype(jnp.bfloat16)
    scaled_rows = jnp.concatenate([scaled, zero_row], axis=0)
    block_width = hidden_width // N_TP

    def one_expert(item):
        indices, gate_w, up_w, down_w = item
        x_rows = token_rows[indices]
        s_rows = scaled_rows[indices]
        gate = jnp.dot(x_rows, gate_w.T, preferred_element_type=jnp.float32)
        up = jnp.dot(x_rows, up_w.T, preferred_element_type=jnp.float32)
        active, slope = silu_parts(gate)
        hidden = (active * up).astype(jnp.bfloat16)
        dhid = jnp.dot(s_rows, down_w.T, preferred_element_type=jnp.float32)
        partial_value = jnp.sum(hidden.astype(jnp.float32) * dhid, axis=1)
        dgate = (dhid * up * slope).astype(jnp.bfloat16)
        dup = (dhid * active).astype(jnp.bfloat16)
        gate_grad = jnp.dot(dgate.T, x_rows, preferred_element_type=jnp.float32)
        up_grad = jnp.dot(dup.T, x_rows, preferred_element_type=jnp.float32)
        down_grad = jnp.dot(hidden.T, s_rows, preferred_element_type=jnp.float32)
        row_count = x_rows.shape[0]
        dgate_blocks = dgate.astype(jnp.float32).reshape(row_count, N_TP, block_width)
        dup_blocks = dup.astype(jnp.float32).reshape(row_count, N_TP, block_width)
        gate_blocks = gate_w.astype(jnp.float32).reshape(N_TP, block_width, model_width)
        up_blocks = up_w.astype(jnp.float32).reshape(N_TP, block_width, model_width)
        pieces = jnp.einsum('rjf,jfd->jrd', dgate_blocks, gate_blocks) + jnp.einsum('rjf,jfd->jrd', dup_blocks, up_blocks)
        rounded = lax.optimization_barrier(pieces.astype(jnp.bfloat16))
        dtok = jnp.sum(rounded.astype(jnp.float32), axis=0)
        return dtok, partial_value, gate_grad, up_grad, down_grad

    dtok_all, partial_all, grad_gate, grad_up, grad_down = lax.map(one_expert, (index_table, w_gate, w_up, w_down))
    dtok_slots = dtok_all[flat_ids, position]
    grad_tokens = jnp.sum(dtok_slots.reshape(token_total, 2, model_width), axis=1).astype(jnp.bfloat16)
    grad_route = (partial_all[flat_ids, position] / weight_flat).reshape(token_total, 2)
    gate_row_norms = jnp.sum(grad_gate * grad_gate, axis=1)
    up_row_norms = jnp.sum(grad_up * grad_up, axis=1)
    down_row_norms = jnp.sum(grad_down * grad_down, axis=2)
    return (grad_tokens, grad_route, grad_gate, grad_up, grad_down, gate_row_norms, up_row_norms, down_row_norms)
```

```python
import functools

import jax
import jax.numpy as jnp
from jax import lax
from jax.experimental import pallas as pl
from jax.experimental.pallas import tpu as pltpu
from jax.sharding import PartitionSpec as P

MESH = pl.DeviceIdType.MESH
F32 = jnp.float32
BF16 = jnp.bfloat16
VMEM_LIMIT = 24 * 2**20
DIRECT = (0, 1,)
ORDER = (
    "A0", "W", "A1", "B0", "C0", "A2", "A3", "B1", "C1", "X", "B2n", "B3n",
    "G02", "B2s", "B3s", "C2", "C3", "K02", "F1", "n24", "F0", "E24", "P", "K24",
    "F3", "R1", "F2", "g0", "H1", "g1", "N", "H0", "g2", "N1", "R2", "H3",
    "H2", "N2",
)
NT = (((1,), (1,)), ((), ()))
VMEM = pl.BlockSpec(memory_space=pltpu.VMEM)
ANY = pl.BlockSpec(memory_space=pl.ANY)
HBM = pl.BlockSpec(memory_space=pltpu.HBM)


def peers(j):
    core, x, y = j % 2, (j // 2) % 2, j // 4
    partner = j + 1 - 2 * core
    xnb = j + 2 - 4 * x
    ynb = j + 4 - 8 * y
    diag = xnb + 4 - 8 * y
    return partner, xnb, ynb, diag


def routing(routes_ref):
    token_count = routes_ref.shape[1]
    r0, r1 = routes_ref[0:1, :], routes_ref[1:2, :]
    eid = lax.broadcasted_iota(jnp.int32, (8, token_count), 0)
    m0, m1 = eid == r0, eid == r1
    m = jnp.logical_or(m0, m1)
    upper = (
        lax.broadcasted_iota(jnp.int32, (token_count, token_count), 0)
        < lax.broadcasted_iota(jnp.int32, (token_count, token_count), 1)
    )
    earlier = jnp.dot(
        jnp.where(m, 1.0, 0.0).astype(BF16),
        jnp.where(upper, 1.0, 0.0).astype(BF16),
        preferred_element_type=F32,
    )
    slot = jnp.where(m, earlier, -1.0)
    return m0, m1, slot


def slot_mask(slot, e, capacity):
    token_count = slot.shape[1]
    ids = lax.broadcasted_iota(jnp.int32, (capacity, token_count), 0).astype(F32)
    return slot[e : e + 1, :] == ids


def signal_all(barrier, devices):
    for device in devices:
        pl.semaphore_signal(barrier, inc=1, device_id=device, device_id_type=MESH)


def remote(src, dst, send_sem, recv_sem, device):
    return pltpu.make_async_remote_copy(
        src_ref=src,
        dst_ref=dst,
        send_sem=send_sem,
        recv_sem=recv_sem,
        device_id=device,
        device_id_type=MESH,
    )


def mirrored(side, plane):
    return plane + side * (3 - 2 * plane)


def swapped(near, plane):
    return plane + near * (2 * ((3 - plane) // 3) - (4 - plane) // 3)


def source_of(i, k):
    side = i // 2
    return mirrored(side, swapped(mirrored(side, i), k))


def chunk_of(i, source):
    side = i // 2
    return swapped(mirrored(side, i), mirrored(side, source))


def targets_of(i):
    side = i // 2
    near = mirrored(side, i)
    return [mirrored(side, e) for e in (near + 1, 3 - 3 * near, near + 2)]


def step_kernel(
    n_ep, n_tp, capacity, routes_hbm, weights_hbm, tok_hbm, go_hbm, wg_hbm, wu_hbm, wd_hbm,
    gg, gu, gd, z_in, route_in, norm_total, down_out, routes_ref, weights_ref,
    full, send_buf, tok_ref, go_ref, wgu, wd, w_own, w_peer, acc, mine, lhs_ref, pair_out, pair_in, chip_sum, plane_in,
    z_out, part_out, part_pair, part_sum, part_in, part_z, norm_out, norm_pair, norm_sum, norm_in,
    load_sem, one_send, one_recv, zr, ts, tr, pr, pair_r, plane_r,
):
    i, j = lax.axis_index("ep"), lax.axis_index("tp")
    width = tok_ref.shape[1]
    hidden_dev, model_width = wd.shape
    n_chip = n_tp // 2
    core = j % 2
    partner, xnb, ynb, diag = peers(j)
    barrier = pltpu.get_barrier_semaphore()
    greet = [(lax.rem(i + d, n_ep), j) for d in range(1, n_ep)]
    greet += [(i, device) for device in (partner, xnb, ynb, diag)]
    signal_all(barrier, greet)
    loads = []
    for index, (source, target) in enumerate((
        (routes_hbm, routes_ref), (weights_hbm, weights_ref), (tok_hbm, tok_ref),
        (go_hbm, go_ref), (wg_hbm, wgu.at[0:hidden_dev]),
        (wu_hbm, wgu.at[hidden_dev : 2 * hidden_dev]), (wd_hbm, wd),
    )):
        load = pltpu.make_async_copy(source, target, load_sem.at[index])
        load.start()
        loads.append(load)

    def cols_at(t):
        return pl.ds(pl.multiple_of(t * width, width), width)

    def rows_of(k):
        return slice(k * capacity, (k + 1) * capacity)

    def block(p, k, col):
        return full.at[p, rows_of(k), cols_at(col)]

    for load in loads[:4]:
        load.wait()
    with jax.named_scope("pick"):
        m0, m1, slot = routing(routes_ref)
        weight = jnp.where(m0, weights_ref[0:1, :], 0.0) + jnp.where(m1, weights_ref[1:2, :], 0.0)
        for e in range(n_ep):
            mask = slot_mask(slot, e, capacity)
            pick = jnp.where(mask, 1.0, 0.0).astype(BF16)
            rows = jnp.dot(pick, tok_ref[...], preferred_element_type=F32)
            grads = jnp.dot(pick, go_ref[...], preferred_element_type=F32)
            scale = jnp.sum(jnp.where(mask, weight[e : e + 1, :], 0.0), axis=1, keepdims=True)
            send_buf[e, 0] = rows.astype(BF16)
            send_buf[e, 1] = (grads * scale).astype(BF16)
        full.at[:, rows_of(0), cols_at(j)][...] = send_buf[i]
    with jax.named_scope("barrier"):
        pl.semaphore_wait(barrier, len(greet))

    def z_copy(p, e):
        k = chunk_of(e, i)
        target = full.at[p, pl.ds(pl.multiple_of(k * capacity, capacity), capacity), cols_at(j)]
        return remote(send_buf.at[e, p], target, one_send.at[0], zr.at[k - 1, p], (e, j))

    for e in targets_of(i):
        for p in range(2):
            z_copy(p, e).start()

    def push(k, index, p, col, device, far=0):
        landed = pr.at[k, far] if index is None else tr.at[k, index]
        remote(block(p, k, col), block(p, k, col), ts.at[k], landed, (i, device)).start()

    def heard(k, index, p, col):
        remote(block(p, k, col), block(p, k, col), ts.at[k], tr.at[k, index], (i, xnb)).wait_recv()

    def spread(k):
        with jax.named_scope(f"A{k}"):
            for p in range(2):
                if k > 0:
                    mine = block(p, k, j)
                    remote(mine, mine, one_send.at[0], zr.at[k - 1, p], (i, xnb)).wait_recv()
                push(k, 2 * p, p, j, xnb)
                push(k, 2 * p + 1, p, j, ynb)
                if k in DIRECT:
                    push(k, 4 + p, p, j, diag)
                else:

                    @pl.when(core == 0)
                    def _(p=p):
                        push(k, 4 + p, p, j, diag)

                push(k, None, p, j, partner)

    def forward(k):
        with jax.named_scope(f"B{k}"):
            for p in range(2):
                for index, col, device in ((2 * p, xnb, ynb), (2 * p + 1, ynb, xnb)):
                    heard(k, index, p, col)
                    if k not in DIRECT and index in (0, 3):

                        @pl.when(core == 1)
                        def _(p=p, col=col, device=device):
                            push(k, 4 + p, p, col, device)

                    push(k, None, p, col, partner)

    def relay(k):
        with jax.named_scope(f"C{k}"):
            heard(k, 4, 0, diag)
            push(k, None, 0, diag, partner, 1)
            heard(k, 5, 1, diag)
            push(k, None, 1, diag, partner, 1)

    def relayed(k, far):
        with jax.named_scope(f"D{k}_{far}"):
            half = full.at[:, rows_of(k), 0 : (1 if far else 3) * width]
            remote(half, half, ts.at[k], pr.at[k, far], (i, partner)).wait_recv()

    def products(rows, chip):
        cols = pl.ds(pl.multiple_of(chip * 2 * width, 2 * width), 2 * width)
        return (
            lax.dot_general(full[0, rows, cols], wgu[:, cols], NT, preferred_element_type=F32),
            lax.dot_general(full[1, rows, cols], wd[:, cols], NT, preferred_element_type=F32),
        )

    def start_compute(first, last):
        for k in range(first, last):
            relayed(k, 0)
        with jax.named_scope(f"n{first}_{last}"):
            rows = slice(first * capacity, last * capacity)
            sums = [products(rows, chip // 2) for chip in (j, xnb, ynb)]
            both, dhid = (a + b + c for a, b, c in zip(*sums))
            acc[rows, 0 : 2 * hidden_dev] = both
            acc[rows, 2 * hidden_dev :] = dhid

    def compute(first, last, started=False):
        for k in range(first, last):
            for far in range(1 if started else 0, 2):
                relayed(k, far)
        with jax.named_scope(f"G{first}_{last}"):
            rows = slice(first * capacity, last * capacity)
            if started:
                both, dhid = products(rows, diag // 2)
                both = both + acc[rows, 0 : 2 * hidden_dev]
                dhid = dhid + acc[rows, 2 * hidden_dev :]
            else:
                both = lax.dot_general(full[0, rows, :], wgu[...], NT, preferred_element_type=F32)
                dhid = lax.dot_general(full[1, rows, :], wd[...], NT, preferred_element_type=F32)
            gate, up = both[:, 0:hidden_dev], both[:, hidden_dev:]
            sig = 1.0 / (1.0 + jnp.exp(-gate))
            active = gate * sig
            slope = sig * (1.0 + gate * (1.0 - sig))
            hidden_f = (active * up).astype(BF16).astype(F32)
            dgate_f = dhid * up * slope
            dup_f = dhid * active
            pair = jnp.concatenate([dgate_f.astype(BF16), dup_f.astype(BF16)], axis=1)
            pair_out[rows, :] = pair
            remote(
                pair_out.at[rows], pair_in.at[rows],
                one_send.at[1], pair_r.at[first], (i, partner),
            ).start()
            mine[rows, :] = jnp.dot(pair, w_own[...], preferred_element_type=F32)
            lhs_ref[0, :, rows] = dgate_f.T.astype(BF16)
            lhs_ref[1, :, rows] = dup_f.T.astype(BF16)
            lhs_ref[2, :, rows] = hidden_f.T.astype(BF16)
            terms = hidden_f * dhid
            for k in range(first, last):
                part = terms[(k - first) * capacity : (k - first + 1) * capacity, :]
                part_out[k : k + 1, 0:capacity] = jnp.sum(part.T, axis=0, keepdims=True)

    def finish_compute(first, last):
        with jax.named_scope(f"K{first}_{last}"):
            rows = slice(first * capacity, last * capacity)
            remote(
                pair_in.at[rows], pair_in.at[rows],
                one_send.at[1], pair_r.at[first], (i, partner),
            ).wait_recv()
            total = mine[rows, :] + jnp.dot(
                pair_in[rows, :], w_peer[...], preferred_element_type=F32
            )
            for k in range(first, last):
                part = total[(k - first) * capacity : (k - first + 1) * capacity, :]
                for q in range(n_chip):
                    chip_sum[k, q] = part[:, q * width : (q + 1) * width].astype(BF16)

    def chip_reduce(k):
        with jax.named_scope(f"F{k}"):
            for kind, target in enumerate((diag, xnb, ynb)):
                remote(
                    chip_sum.at[k, target // 2], plane_in.at[k, kind],
                    one_send.at[2], plane_r.at[k], (i, target),
                ).start()

    def plane_reduce(k):
        with jax.named_scope(f"H{k}"):
            remote(
                plane_in.at[k], plane_in.at[k], one_send.at[2], plane_r.at[k], (i, xnb)
            ).wait_recv()
            done = (
                chip_sum[k, j // 2].astype(F32)
                + plane_in[k, 0].astype(F32)
                + plane_in[k, 1].astype(F32)
                + plane_in[k, 2].astype(F32)
            ).astype(BF16)
            if k == 0:
                z_in[i] = done
            else:
                z_out[k - 1] = done
                remote(
                    z_out.at[k - 1], z_in.at[i], one_send.at[3], one_recv.at[0],
                    (source_of(i, k), j),
                ).start()

    def load_weights():
        for load in loads[4:]:
            load.wait()
        for q in range(n_chip):
            block_cols = slice(q * width, (q + 1) * width)
            remote(
                wgu.at[:, cols_at(2 * q + 1 - core)], w_peer.at[:, block_cols],
                one_send.at[9], one_recv.at[6], (i, partner),
            ).start()
            w_own[:, block_cols] = wgu[:, cols_at(2 * q + core)]

    def peer_weights():
        with jax.named_scope("X"):
            remote(w_peer, w_peer, one_send.at[9], one_recv.at[6], (i, partner)).wait_recv()

    part_copy = remote(part_out, part_pair, one_send.at[4], one_recv.at[1], (i, partner))
    norm_copy = remote(norm_out, norm_pair, one_send.at[6], one_recv.at[3], (i, partner))

    def route_chip():
        with jax.named_scope("R1"):
            part_copy.wait_recv()
            part_sum[...] = part_out[...] + part_pair[...]
            for kind, target in enumerate((diag, xnb, ynb)):
                remote(
                    part_sum, part_in.at[kind], one_send.at[5], one_recv.at[2], (i, target)
                ).start()

    def route_plane():
        with jax.named_scope("R2"):
            remote(part_in, part_in, one_send.at[5], one_recv.at[2], (i, xnb)).wait_recv()
            total = part_sum[...] + part_in[0] + part_in[1] + part_in[2]
            part_z[...] = total
            route_in[i] = total
            for d in range(1, n_ep):
                remote(
                    part_z, route_in.at[i], one_send.at[7], one_recv.at[4],
                    (lax.rem(i + d, n_ep), j),
                ).start()

    def norm_chip():
        with jax.named_scope("N1"):
            norm_copy.wait_recv()
            norm_sum[...] = norm_out[...] + norm_pair[...]
            for kind, target in enumerate((diag, xnb, ynb)):
                remote(
                    norm_sum, norm_in.at[kind], one_send.at[8], one_recv.at[5], (i, target)
                ).start()

    def norm_plane():
        with jax.named_scope("N2"):
            remote(norm_in, norm_in, one_send.at[8], one_recv.at[5], (i, xnb)).wait_recv()
            norm_total[...] = norm_sum[...] + norm_in[0] + norm_in[1] + norm_in[2]

    rows_norm = model_width // 128
    tile = 512

    def weight_grad(index, rhs, out):
        with jax.named_scope(f"grad{index}"):
            sums = jnp.zeros((out.shape[0], 128), F32)
            for n in range(model_width // tile):
                cols = slice(n * tile, (n + 1) * tile)
                grad = jnp.dot(lhs_ref[index], full[rhs, :, cols], preferred_element_type=F32)
                out[:, cols] = grad
                square = grad * grad
                if rhs == 0:
                    norm = jnp.sum(square, axis=0, keepdims=True)
                    for q in range(tile // 128):
                        row = index * rows_norm + n * (tile // 128) + q
                        norm_out[row : row + 1, :] = norm[:, q * 128 : (q + 1) * 128]
                else:
                    for q in range(tile // 128):
                        sums = sums + square[:, q * 128 : (q + 1) * 128]
            if rhs == 1:
                down_out[...] = jnp.sum(sums.T, axis=0, keepdims=True)

    part_out[...] = jnp.zeros_like(part_out)
    steps = {
        "A": spread, "B": forward, "C": relay, "F": chip_reduce, "H": plane_reduce,
    }
    others = {
        "W": load_weights,
        "X": peer_weights,
        "P": part_copy.start,
        "R1": route_chip,
        "R2": route_plane,
        "g0": lambda: weight_grad(0, 0, gg),
        "g1": lambda: weight_grad(1, 0, gu),
        "g2": lambda: weight_grad(2, 1, gd),
        "N": norm_copy.start,
        "N1": norm_chip,
        "N2": norm_plane,
    }
    for name in ORDER:
        if name in others:
            others[name]()
        elif name[0] == "K":
            finish_compute(int(name[1]), int(name[2]))
        elif name[0] == "n":
            start_compute(int(name[1]), int(name[2]))
        elif name[0] in "GE":
            compute(int(name[1]), int(name[2]), name[0] == "E")
        else:
            step, k = steps[name[0]], int(name[1])
            if len(name) == 2:
                step(k)
            else:

                @pl.when(core == "sn".index(name[2]))
                def _(step=step, k=k):
                    step(k)

    with jax.named_scope("zret"):
        remote(part_in, part_in, one_send.at[7], one_recv.at[4], (i, xnb)).wait_recv()
        remote(z_out, z_out, one_send.at[3], one_recv.at[0], (i, xnb)).wait_recv()
    with jax.named_scope("drain"):
        part_copy.wait_send()
        norm_copy.wait_send()
        for k in range(n_ep):
            sent = full.at[:, rows_of(k), 0 : 7 * width]
            remote(sent, sent, ts.at[k], pr.at[k, 0], (i, xnb)).wait_send()
        for sent, index in (
            (send_buf.at[0:3], 0), (pair_in, 1), (plane_in, 2), (z_out, 3), (part_in, 5),
            (part_in, 7), (norm_in, 8), (w_peer, 9),
        ):
            remote(sent, sent, one_send.at[index], one_recv.at[0], (i, xnb)).wait_send()


def finish_kernel(
    n_ep, capacity, gg, gu, gd, z_in, route_in, norm_total, down_sums, routes_ref, weights_ref,
    gg_hbm, gu_hbm, gd_hbm, gt_hbm, gr_hbm, gn_hbm, un_hbm, dn_hbm,
    gt_ref, gr_ref, gn_ref, un_ref, out_sem, small_sem,
):
    hidden_dev, model_width = gg.shape
    tile = hidden_dev // out_sem.shape[1]
    stores = []
    for index, (buf, out) in enumerate(((gg, gg_hbm), (gu, gu_hbm), (gd, gd_hbm))):
        for n in range(out_sem.shape[1]):
            rows = slice(n * tile, (n + 1) * tile)
            store = pltpu.make_async_copy(buf.at[rows], out.at[rows], out_sem.at[index, n])
            store.start()
            stores.append(store)

    def save(source, target, index):
        store = pltpu.make_async_copy(source, target, small_sem.at[index])
        store.start()
        stores.append(store)

    save(down_sums, dn_hbm, 0)
    rows_norm = model_width // 128
    for r in range(rows_norm):
        gn_ref[:, r * 128 : (r + 1) * 128] = norm_total[r : r + 1, :]
        un_ref[:, r * 128 : (r + 1) * 128] = norm_total[rows_norm + r : rows_norm + r + 1, :]
    save(gn_ref, gn_hbm, 1)
    save(un_ref, un_hbm, 2)

    i = lax.axis_index("ep")
    m0, m1, slot = routing(routes_ref)
    acc = jnp.zeros(gt_ref.shape, F32)
    back_route = []
    for e in range(n_ep):
        pick = jnp.where(slot_mask(slot, e, capacity), 1.0, 0.0)
        acc = acc + jnp.dot(pick.T.astype(BF16), z_in[e], preferred_element_type=F32)
        values = route_in[e, pl.ds(chunk_of(e, i), 1), :][:, 0:capacity]
        back_route.append(
            jnp.dot(
                values, pick, preferred_element_type=F32, precision=lax.Precision.HIGHEST
            )
        )
    gt_ref[...] = acc.astype(BF16)
    save(gt_ref, gt_hbm, 3)
    for k, m in enumerate((m0, m1)):
        value = jnp.zeros_like(back_route[0])
        for e in range(n_ep):
            value = value + jnp.where(m[e : e + 1, :], back_route[e], 0.0)
        gr_ref[k : k + 1, :] = value / weights_ref[k : k + 1, :]
    save(gr_ref, gr_hbm, 4)
    for store in stores:
        store.wait()


def per_device_kernels(tokens, routes, route_weights, grad_out, w_gate, w_up, w_down):
    token_count, width = tokens.shape
    _, hidden_dev, model_width = w_gate.shape
    n_ep, n_tp = lax.axis_size("ep"), lax.axis_size("tp")
    n_chip = n_tp // 2
    capacity = min(3 * token_count // n_ep, token_count // 2)
    rows = n_ep * capacity
    block = (capacity, width)
    norm_rows = 2 * (model_width // 128)
    dma = pltpu.SemaphoreType.DMA
    part = pltpu.VMEM((8, 128), F32)
    norm = pltpu.VMEM((norm_rows, 128), F32)
    grad = pltpu.VMEM((hidden_dev, model_width), F32)
    inner = pl.pallas_call(
        functools.partial(step_kernel, n_ep, n_tp, capacity),
        name="step",
        out_shape=(
            *[grad] * 3,
            pltpu.VMEM((n_ep, *block), BF16),
            pltpu.VMEM((n_ep, 8, 128), F32),
            norm,
            pltpu.VMEM((1, hidden_dev), F32),
            pltpu.VMEM((2, token_count), jnp.int32),
            pltpu.VMEM((2, token_count), F32),
        ),
        in_specs=[HBM] * 7,
        out_specs=[VMEM] * 9,
        scratch_shapes=[
            pltpu.VMEM((2, rows, model_width), BF16),
            pltpu.VMEM((n_ep, 2, *block), BF16),
            *[pltpu.VMEM((token_count, width), BF16)] * 2,
            pltpu.VMEM((2 * hidden_dev, model_width), BF16),
            pltpu.VMEM((hidden_dev, model_width), BF16),
            *[pltpu.VMEM((2 * hidden_dev, model_width // 2), BF16)] * 2,
            pltpu.VMEM((rows, 3 * hidden_dev), F32),
            pltpu.VMEM((rows, model_width // 2), F32),
            pltpu.VMEM((3, hidden_dev, rows), BF16),
            *[pltpu.VMEM((rows, 2 * hidden_dev), BF16)] * 2,
            pltpu.VMEM((n_ep, n_chip, *block), BF16),
            pltpu.VMEM((n_ep, 3, *block), BF16),
            pltpu.VMEM((n_ep - 1, *block), BF16),
            part, part, part, pltpu.VMEM((3, 8, 128), F32), part,
            norm, norm, norm, pltpu.VMEM((3, norm_rows, 128), F32),
            dma((7,)),
            dma((10,)),
            dma((7,)),
            dma((n_ep - 1, 2)),
            dma((n_ep,)),
            dma((n_ep, 6)),
            dma((n_ep, 2)),
            *[dma((n_ep,))] * 2,
        ],
        compiler_params=pltpu.CompilerParams(
            collective_id=0, has_side_effects=True, vmem_limit_bytes=VMEM_LIMIT
        ),
    )(*[
        pltpu.with_memory_space_constraint(operand, pltpu.HBM)
        for operand in (
            routes.T, route_weights.T, tokens, grad_out, w_gate[0], w_up[0], w_down[0]
        )
    ])

    grad_shape = jax.ShapeDtypeStruct((hidden_dev, model_width), F32)
    norm_shape = jax.ShapeDtypeStruct((1, model_width), F32)
    grad_gate, grad_up, grad_down, grad_tokens, grad_route, gate_norms, up_norms, down_norms = (
        pl.pallas_call(
            functools.partial(finish_kernel, n_ep, capacity),
            name="finish",
            out_shape=(
                *[grad_shape] * 3,
                jax.ShapeDtypeStruct((token_count, width), BF16),
                jax.ShapeDtypeStruct((2, token_count), F32),
                *[norm_shape] * 2,
                jax.ShapeDtypeStruct((1, hidden_dev), F32),
            ),
            in_specs=[VMEM] * 9,
            out_specs=[ANY] * 8,
            scratch_shapes=[
                pltpu.VMEM((token_count, width), BF16),
                pltpu.VMEM((2, token_count), F32),
                *[pltpu.VMEM((1, model_width), F32)] * 2,
                dma((3, 4)),
                dma((5,)),
            ],
            compiler_params=pltpu.CompilerParams(vmem_limit_bytes=VMEM_LIMIT),
        )(*inner)
    )
    return (
        grad_tokens,
        grad_route.T,
        grad_gate[None],
        grad_up[None],
        grad_down[None],
        gate_norms,
        up_norms,
        down_norms,
    )


def silu_parts(pre_act):
    sigmoid_val = jax.nn.sigmoid(pre_act)
    return (pre_act * sigmoid_val, sigmoid_val * (1.0 + pre_act * (1.0 - sigmoid_val)))


def per_device(tokens, routes, route_weights, grad_out, w_gate, w_up, w_down):
    token_count, feature_dev = tokens.shape
    experts_dev, hidden_dev, model_width = w_gate.shape
    ep_size = lax.axis_size("ep")
    expert_total = experts_dev * ep_size
    capacity = min(3 * token_count // expert_total, token_count // 2)
    slot_count = expert_total * capacity
    row_count = ep_size * capacity
    flat_ids = routes.reshape(-1)
    pair_count = flat_ids.shape[0]
    one_hot = (flat_ids[:, None] == jnp.arange(expert_total, dtype=jnp.int32)[None, :]).astype(
        jnp.bfloat16
    )
    lower = (
        jnp.arange(pair_count, dtype=jnp.int32)[:, None]
        > jnp.arange(pair_count, dtype=jnp.int32)[None, :]
    ).astype(jnp.bfloat16)
    earlier = jnp.dot(lower, one_hot, preferred_element_type=jnp.float32)
    slot_ids = jnp.sum(earlier * one_hot.astype(jnp.float32), axis=1).astype(jnp.int32)
    position = flat_ids % experts_dev * row_count + flat_ids // experts_dev * capacity + slot_ids
    dispatch = (position[None, :] == jnp.arange(slot_count, dtype=jnp.int32)[:, None]).astype(
        jnp.bfloat16
    )
    weight_flat = route_weights.reshape(-1)
    token_rows = jnp.repeat(tokens, 2, axis=0)
    scaled = (weight_flat[:, None] * jnp.repeat(grad_out, 2, axis=0).astype(jnp.float32)).astype(
        jnp.bfloat16
    )
    send_shape = (experts_dev, ep_size, capacity, feature_dev)
    x_send = (
        jnp.dot(dispatch, token_rows, preferred_element_type=jnp.float32)
        .astype(jnp.bfloat16)
        .reshape(send_shape)
    )
    s_send = (
        jnp.dot(dispatch, scaled, preferred_element_type=jnp.float32)
        .astype(jnp.bfloat16)
        .reshape(send_shape)
    )
    x_recv, s_recv = (
        lax.all_to_all(x_send, "ep", split_axis=1, concat_axis=1, tiled=True),
        lax.all_to_all(s_send, "ep", split_axis=1, concat_axis=1, tiled=True),
    )
    x_full, s_full = (
        lax.all_gather(x_recv, "tp", axis=3, tiled=True),
        lax.all_gather(s_recv, "tp", axis=3, tiled=True),
    )
    x_rows = x_full.reshape(experts_dev, row_count, model_width)
    s_rows = s_full.reshape(experts_dev, row_count, model_width)
    gate = jnp.einsum("erd,efd->erf", x_rows, w_gate, preferred_element_type=jnp.float32)
    up = jnp.einsum("erd,efd->erf", x_rows, w_up, preferred_element_type=jnp.float32)
    dhid = jnp.einsum("erd,efd->erf", s_rows, w_down, preferred_element_type=jnp.float32)
    active, slope = silu_parts(gate)
    hidden = (active * up).astype(jnp.bfloat16)
    partial_value = jnp.sum(hidden.astype(jnp.float32) * dhid, axis=2)
    dgate = (dhid * up * slope).astype(jnp.bfloat16)
    dup = (dhid * active).astype(jnp.bfloat16)
    grad_gate = jnp.einsum("erf,erd->efd", dgate, x_rows, preferred_element_type=jnp.float32)
    grad_up = jnp.einsum("erf,erd->efd", dup, x_rows, preferred_element_type=jnp.float32)
    grad_down = jnp.einsum("erf,erd->efd", hidden, s_rows, preferred_element_type=jnp.float32)
    back_terms = jnp.einsum("erf,efd->erd", dgate, w_gate, preferred_element_type=jnp.float32)
    back_terms = back_terms + jnp.einsum(
        "erf,efd->erd", dup, w_up, preferred_element_type=jnp.float32
    )
    back_terms = back_terms.reshape(experts_dev, ep_size, capacity, model_width)
    gate_norms = jnp.sum(grad_gate * grad_gate, axis=1)
    up_norms = jnp.sum(grad_up * grad_up, axis=1)
    down_norms = jnp.sum(grad_down * grad_down, axis=2)
    partial_value, gate_norms, up_norms = lax.psum((partial_value, gate_norms, up_norms), "tp")
    partial_sent = partial_value.reshape(experts_dev, ep_size, capacity)
    dtok_mine = lax.psum_scatter(
        back_terms.astype(jnp.bfloat16), "tp", scatter_dimension=3, tiled=True
    ).astype(jnp.float32)
    returned, partial_back = (
        lax.all_to_all(
            dtok_mine.astype(jnp.bfloat16), "ep", split_axis=1, concat_axis=1, tiled=True
        ).astype(dtok_mine.dtype),
        lax.all_to_all(
            partial_sent.astype(jnp.bfloat16), "ep", split_axis=1, concat_axis=1, tiled=True
        ).astype(partial_sent.dtype),
    )
    slot_rows = jnp.take(returned.reshape(slot_count, feature_dev), position, axis=0)
    grad_tokens = jnp.sum(slot_rows.reshape(token_count, 2, feature_dev), axis=1).astype(
        jnp.bfloat16
    )
    slot_partial = jnp.take(partial_back.reshape(slot_count), position, axis=0)
    grad_route = (slot_partial / weight_flat).reshape(token_count, 2)
    return (
        grad_tokens,
        grad_route,
        grad_gate,
        grad_up,
        grad_down,
        gate_norms,
        up_norms,
        down_norms,
    )


def solution(mesh):
    in_specs = (
        P("ep", "tp"),
        P("ep", None),
        P("ep", None),
        P("ep", "tp"),
        P("ep", "tp", None),
        P("ep", "tp", None),
        P("ep", "tp", None),
    )
    out_specs = (
        P("ep", "tp"),
        P("ep", None),
        P("ep", "tp", None),
        P("ep", "tp", None),
        P("ep", "tp", None),
        P("ep", None),
        P("ep", None),
        P("ep", "tp"),
    )
    fits = mesh.shape["tp"] == 8 and mesh.shape["ep"] == 4
    return jax.shard_map(
        per_device_kernels if fits else per_device, mesh=mesh, in_specs=in_specs, out_specs=out_specs, check_vma=False
    )
```
